256 devices in a mesh: kv: 64 (over z, y, core), tp: 4 (over x).
Axes of the slice: x: 4, y: 4, z: 8, core: 2. Of those that a mesh axis runs over, the one named last changes fastest.
Arguments:
- queries: bfloat16 [24576, 2048], P('kv', 'tp'), may hold values from -3 to 3
- key_heads: bfloat16 [24576, 512], P('kv', 'tp'), may hold values from -3 to 3
- values: bfloat16 [24576, 512], P('kv', 'tp'), may hold values from -6 to 6
- log_sums: float32 [32, 24576], P('tp', 'kv'), may hold values from 4 to 6
- out_grad: bfloat16 [24576, 2048], P('kv', 'tp'), may hold values from -12 to 12
- inputs: bfloat16 [24576, 4096], P('kv', 'tp'), may hold values from -0.059814453 to 0.059814453
- chosen: int32 [8, 384, 16], P('tp'), may hold values from -1 to 383, as said below
Outputs:
- query_grad: float32 [24576, 2048], P('kv', 'tp')
- key_grad: float32 [24576, 512], P('kv', 'tp')
- value_grad: float32 [24576, 512], P('kv', 'tp')
- weight_grad: float32 [4096, 512], P('kv', 'tp')
The draws below stay inside these ranges and needn't reach their ends.
Inputs may be any that keep to these rules, and one draw needn't show every extreme that they name: `chosen`: for each key-value head and query block the used entries come first, are distinct, and none is above the query block's own number; -1 fills the rest. Up to 16 entries are used, all of them in some query blocks. For one key-value head, the query blocks held by one index of kv list at most one block of each other index of kv, and every index of kv but the first lists a block of the first.
All inputs are finite; a program needn't handle non-finite values.
Results may differ from the reference program's by a relative error of at most 0.014.
Values may be sent and summed in bfloat16 or wider, within the bound.
No kernel may reach another device: no remote copies, remote signals or barrier semaphores. Data moves between devices by JAX's collectives and lax.ppermute only.
A program may use at most 128 MiB of HBM per device.

```python
import jax
import jax.numpy as jnp
from jax import lax

D = 4096
HEADS = 32
KV_HEADS = 8
HD = 64
BLOCK = 64
CHOSEN = 16
TOK_DEV = 384
TOKENS = 24576


def draw_chosen(key, part):
    per_device = TOK_DEV // BLOCK
    devices = TOKENS // TOK_DEV
    total_blocks = TOKENS // BLOCK
    subkeys = jax.random.split(jax.random.fold_in(key, 17), 4)
    designated = jax.random.randint(subkeys[0], (KV_HEADS, devices, devices), 0, per_device)
    requester_pos = jnp.arange(devices)[None, :, None]
    owner_pos = jnp.arange(devices)[None, None, :]
    designated = jnp.where(owner_pos == 0, 0, designated)
    designated = jnp.where(owner_pos == requester_pos - 1, per_device - 1, designated)
    query_block = jnp.arange(total_blocks)[:, None]
    other_block = jnp.arange(total_blocks)[None, :]
    requester = query_block // per_device
    owner_of = other_block // per_device
    within_dev = other_block % per_device
    chosen_here = designated[:, requester, owner_of]
    remote_ok = (owner_of < requester)[None] & (within_dev[None] == chosen_here)
    local_ok = ((owner_of == requester) & (other_block <= query_block))[None]
    allowed = remote_ok | local_ok
    last_local = query_block % per_device == per_device - 1
    forced = (other_block == 0) | (other_block == query_block) | (other_block == query_block - 1)
    forced = forced | (owner_of == requester - devices // 2) & last_local
    forced = forced[None] & allowed
    popularity = jax.random.randint(subkeys[1], (KV_HEADS, 1, total_blocks), 0, 4)
    noise_bits = jax.random.randint(subkeys[2], (KV_HEADS, total_blocks, total_blocks), 0, 65536)
    level = jnp.where(forced, 7, popularity)
    ranking = jnp.where(allowed, (level * 65536 + noise_bits) * total_blocks + other_block[None], -1 - other_block[None])
    top_score, top_index = lax.top_k(ranking, CHOSEN)
    list_length = CHOSEN // 2 + jax.random.randint(subkeys[3], (KV_HEADS, total_blocks, 1), 0, CHOSEN - CHOSEN // 2 + 1)
    list_length = jnp.where(last_local[None], CHOSEN, list_length)
    slot_pos = jnp.arange(CHOSEN)[None, None, :]
    keep_slot = (slot_pos < list_length) & (top_score >= 0)
    return jnp.where(keep_slot, top_index, -1).astype(jnp.int32)


def shard_levels(key, extent, cuts, smallest, high):
    gain, own = 1.0, jax.random.fold_in(key, 6)
    for axis_at, parts in cuts:
        heights = jnp.exp(jax.random.uniform(jax.random.fold_in(own, axis_at), (parts,), jnp.float32, smallest / len(cuts), high / len(cuts)))
        gain = gain * jnp.repeat(heights, extent[axis_at] // parts).reshape([-1 if axis == axis_at else 1 for axis in range(len(extent))])
    return gain


def normal_values(stream_key, extent, deviation, most, cuts=(), kind=jnp.bfloat16):
    loudness = shard_levels(stream_key, extent, cuts, -0.22, 0.18) if cuts else 1.0
    array = jax.random.normal(stream_key, extent, jnp.float32) * deviation * loudness
    return jnp.minimum(jnp.maximum(array, -most), most).astype(kind)


def setup_inputs(seed: int = 0) -> dict:
    splits = jax.random.split(jax.random.key(seed), 8)
    queries = normal_values(splits[0], (TOKENS, HEADS * HD), 1.0, 3.0, ((0, 64), (1, 4)))
    key_heads = normal_values(splits[1], (TOKENS, KV_HEADS * HD), 1.0, 3.0, ((0, 64), (1, 4)))
    values = normal_values(splits[2], (TOKENS, KV_HEADS * HD), 1.0, 6.0, ((0, 64), (1, 4)))
    log_sums = jnp.clip(4.0 + 2.0 * jax.random.uniform(splits[3], (HEADS, TOKENS), jnp.float32) ** shard_levels(splits[3], (HEADS, TOKENS), ((0, 4), (1, 64)), -0.2, 0.2), 4.0, 6.0)
    out_grad = normal_values(splits[4], (TOKENS, HEADS * HD), 2.0, 12.0, ((0, 64), (1, 4)))
    inputs = normal_values(splits[5], (TOKENS, D), 0.01, 0.059814453, ((0, 64), (1, 4)))
    chosen = draw_chosen(jax.random.fold_in(splits[7], 71), 0)
    return {"queries": queries, "key_heads": key_heads, "values": values, "log_sums": log_sums, "out_grad": out_grad, "inputs": inputs, "chosen": chosen}


def reference(queries, key_heads, values, log_sums, out_grad, inputs, chosen):
    total_blocks = TOKENS // BLOCK
    per_group = HEADS // KV_HEADS
    scaling = HD ** -0.5
    kv_pairs = jnp.concatenate(
        [key_heads.reshape(TOKENS, KV_HEADS, HD), values.reshape(TOKENS, KV_HEADS, HD)], axis=2
    ).reshape(total_blocks, BLOCK, KV_HEADS, 2 * HD)
    group_col = jnp.arange(KV_HEADS, dtype=jnp.int32)[:, None]
    offsets = jnp.arange(BLOCK, dtype=jnp.int32)

    def one_block(totals, block_pos):
        block_list = lax.dynamic_index_in_dim(chosen, block_pos, 1, keepdims=False)
        list_valid = block_list >= 0
        safe_list = jnp.maximum(block_list, 0)
        fetched = kv_pairs[safe_list, :, group_col, :].reshape(KV_HEADS, CHOSEN * BLOCK, 2 * HD)
        fetched = fetched.astype(jnp.float32)
        key_part = fetched[..., :HD]
        value_part = fetched[..., HD:]
        first_row = block_pos * BLOCK
        query_part = lax.dynamic_slice_in_dim(queries, first_row, BLOCK, 0)
        query_part = query_part.reshape(BLOCK, KV_HEADS, per_group, HD).astype(jnp.float32)
        grad_part = lax.dynamic_slice_in_dim(out_grad, first_row, BLOCK, 0)
        grad_part = grad_part.reshape(BLOCK, KV_HEADS, per_group, HD).astype(jnp.float32)
        sums_part = lax.dynamic_slice_in_dim(log_sums, first_row, BLOCK, 1).reshape(KV_HEADS, per_group, BLOCK)
        scores = jnp.einsum("igrd,gkd->grik", query_part, key_part) * scaling
        key_pos = (safe_list[:, :, None] * BLOCK + offsets).reshape(KV_HEADS, CHOSEN * BLOCK)
        key_valid = jnp.repeat(list_valid, BLOCK, axis=1)
        query_pos = first_row + offsets
        visible = key_valid[:, None, None, :] & (key_pos[:, None, None, :] <= query_pos[None, None, :, None])
        prob_rows = jnp.where(visible, jnp.exp(scores - sums_part[..., None]), 0.0)
        prob_grad = jnp.einsum("igrd,gkd->grik", grad_part, value_part)
        row_delta = jnp.sum(prob_rows * prob_grad, axis=-1, keepdims=True)
        score_grad = prob_rows * (prob_grad - row_delta)
        prob_half = prob_rows.astype(jnp.bfloat16).astype(jnp.float32)
        score_half = score_grad.astype(jnp.bfloat16).astype(jnp.float32)
        query_part_grad = jnp.einsum("grik,gkd->igrd", score_half, key_part) * scaling
        key_contrib = jnp.einsum("grik,igrd->gkd", score_half, query_part) * scaling
        value_contrib = jnp.einsum("grik,igrd->gkd", prob_half, grad_part)
        contribs = jnp.concatenate([key_contrib, value_contrib], axis=2).reshape(KV_HEADS, CHOSEN, BLOCK, 2 * HD)
        totals = totals.at[safe_list, :, group_col, :].add(contribs)
        return totals, query_part_grad.reshape(BLOCK, HEADS * HD)

    start_totals = jnp.zeros((total_blocks, BLOCK, KV_HEADS, 2 * HD), jnp.float32)
    totals, query_blocks = lax.scan(one_block, start_totals, jnp.arange(total_blocks, dtype=jnp.int32))
    query_grad = query_blocks.reshape(TOKENS, HEADS * HD)
    totals = totals.reshape(TOKENS, KV_HEADS, 2 * HD)
    key_grad = totals[..., :HD].reshape(TOKENS, KV_HEADS * HD)
    value_grad = totals[..., HD:].reshape(TOKENS, KV_HEADS * HD)
    weight_grad = jnp.dot(inputs.T, key_grad.astype(jnp.bfloat16), preferred_element_type=jnp.float32)
    return (query_grad, key_grad, value_grad, weight_grad)
```

```python
import jax
import jax.numpy as jnp
from jax import lax
from jax.experimental import pallas as pl
from jax.experimental.pallas import tpu as pltpu
from jax.sharding import PartitionSpec as P

HD = 64
BLOCK = 64
GROUPS = 2
PER_GROUP = 4
BLOCKS = 6
LIST = 16
DEVS = 64
COLS = PER_GROUP * BLOCK
CHUNK = 256
LOG2E = 1.4426950408889634
VMEM = pltpu.VMEM
SMEM = pltpu.SMEM


def vmem_spec():
    return pl.BlockSpec(memory_space=VMEM)


def smem_spec():
    return pl.BlockSpec(memory_space=SMEM)


def pack_kernel(sel_ref, keys_ref, values_ref, out_ref, own_ref):
    shape = (BLOCKS * BLOCK, 2 * HD)
    low = lax.broadcasted_iota(jnp.int32, shape, 1) < HD
    keys = keys_ref[...].astype(jnp.float32)
    values = values_ref[...].astype(jnp.float32)
    first = jnp.where(low, keys, pltpu.roll(values, HD, 1)).astype(jnp.bfloat16)
    second = jnp.where(low, pltpu.roll(keys, HD, 1), values).astype(jnp.bfloat16)
    own_ref[0] = first.reshape(BLOCKS, BLOCK, 2 * HD)
    own_ref[1] = second.reshape(BLOCKS, BLOCK, 2 * HD)

    @pl.loop(0, DEVS)
    def _(dest):
        for group in range(GROUPS):
            out_ref[dest, group] = own_ref[group, sel_ref[group, dest]]


def attention_kernel(
    slot_ref,
    near_ref,
    remote_ref,
    own_ref,
    query_ref,
    grad_ref,
    sums_ref,
    sent_ref,
    kept_ref,
    query_grad_ref,
    totals,
    table,
    probs,
    prob_grads,
):
    totals[...] = jnp.zeros_like(totals)
    rows = lax.broadcasted_iota(jnp.int32, (BLOCK, COLS), 0)
    cols = lax.broadcasted_iota(jnp.int32, (BLOCK, COLS), 1)
    behind = rows - lax.rem(cols, BLOCK)
    nt = (((1,), (1,)), ((), ()))
    tn = (((0,), (0,)), ((), ()))
    nn = (((1,), (0,)), ((), ()))

    @pl.loop(0, GROUPS * BLOCKS)
    def _(step):
        group = step // BLOCKS
        position = lax.rem(step, BLOCKS)
        query = query_ref[step]
        grad = grad_ref[step]
        sums = sums_ref[step]
        for entry in range(LIST):
            slot = slot_ref[step, entry]

            @pl.when(slot < DEVS)
            def _():
                table[pl.ds(entry * BLOCK, BLOCK), :] = remote_ref[slot, group]

            @pl.when(slot >= DEVS)
            def _():
                table[pl.ds(entry * BLOCK, BLOCK), :] = own_ref[group, slot - DEVS]

        delta = jnp.zeros((BLOCK, COLS), jnp.float32)
        for entry in range(LIST):
            part = pl.ds(entry * BLOCK, BLOCK)
            pair = table[part, :]
            score = lax.dot_general(pair, query, nt, preferred_element_type=jnp.float32)
            prob_grad = lax.dot_general(pair, grad, nt, preferred_element_type=jnp.float32)
            prob = jnp.exp2(score * (LOG2E * HD**-0.5) - sums)
            prob = jnp.where(behind <= near_ref[step, entry], prob, 0.0)
            delta = delta + prob * prob_grad
            probs[part, :] = prob
            prob_grads[part, :] = prob_grad
        delta = jnp.sum(delta, axis=0, keepdims=True)
        query_grad = jnp.zeros((2 * HD, COLS), jnp.float32)
        for chunk in range(LIST * BLOCK // CHUNK):
            part = pl.ds(chunk * CHUNK, CHUNK)
            prob = probs[part, :]
            score_grad = (prob * (prob_grads[part, :] - delta)).astype(jnp.bfloat16)
            contrib = lax.dot_general(
                score_grad, query, nn, preferred_element_type=jnp.float32
            ) + lax.dot_general(
                prob.astype(jnp.bfloat16), grad, nn, preferred_element_type=jnp.float32
            )
            query_grad = query_grad + lax.dot_general(
                table[part, :], score_grad, tn, preferred_element_type=jnp.float32
            )
            for inner in range(CHUNK // BLOCK):
                entry = chunk * (CHUNK // BLOCK) + inner
                slot = slot_ref[step, entry]
                totals[slot, group] += contrib[inner * BLOCK : (inner + 1) * BLOCK]
        query_grad_ref[step] = query_grad[:HD] * HD**-0.5

    lane = lax.broadcasted_iota(jnp.int32, (BLOCK, 2 * HD), 1)
    factor = jnp.where(lane < HD, HD**-0.5, 1.0)

    @pl.loop(0, DEVS)
    def _(dest):
        for group in range(GROUPS):
            sent_ref[dest, group] = (totals[dest, group] * factor).astype(jnp.bfloat16)

    for block in range(BLOCKS):
        for group in range(GROUPS):
            kept_ref[group, block] = totals[DEVS + block, group] * factor


def collect_kernel(sel_ref, returned_ref, kept_ref, key_ref, value_ref, half_ref, total):
    total[...] = kept_ref[...]

    @pl.loop(0, DEVS)
    def _(source):
        for group in range(GROUPS):
            total[group, sel_ref[group, source]] += returned_ref[source, group].astype(jnp.float32)

    low = lax.broadcasted_iota(jnp.int32, (BLOCKS * BLOCK, 2 * HD), 1) < HD
    first = total[0].reshape(BLOCKS * BLOCK, 2 * HD)
    second = total[1].reshape(BLOCKS * BLOCK, 2 * HD)
    key_grad = jnp.where(low, first, pltpu.roll(second, HD, 1))
    key_ref[...] = key_grad
    half_ref[...] = key_grad.astype(jnp.bfloat16)
    value_ref[...] = jnp.where(low, pltpu.roll(first, HD, 1), second)


def local(queries, key_heads, values, log_sums, out_grad, inputs, chosen):
    me = lax.axis_index("kv")
    rows = BLOCKS * BLOCK
    first = me * BLOCKS
    within = chosen.reshape(GROUPS, DEVS, BLOCKS * LIST) - first
    listed = (within >= 0) & (within < BLOCKS)
    sel = jnp.max(jnp.where(listed, within, 0), axis=2)
    mine = lax.dynamic_slice_in_dim(chosen, first, BLOCKS, 1)
    near = mine - first
    slot = jnp.where(near >= 0, DEVS + near, jnp.maximum(mine, 0) // BLOCKS)
    positions = jnp.arange(BLOCKS, dtype=jnp.int32)[None, :, None]
    near = jnp.where(mine < 0, -BLOCK, jnp.where(near == positions, 0, BLOCK))
    slot = slot.reshape(GROUPS * BLOCKS, LIST)
    near = near.reshape(GROUPS * BLOCKS, LIST)

    bf16 = jnp.bfloat16
    outgoing, own = pl.pallas_call(
        pack_kernel,
        out_shape=(
            jax.ShapeDtypeStruct((DEVS, GROUPS, BLOCK, 2 * HD), bf16),
            jax.ShapeDtypeStruct((GROUPS, BLOCKS, BLOCK, 2 * HD), bf16),
        ),
        in_specs=[smem_spec(), vmem_spec(), vmem_spec()],
        out_specs=(vmem_spec(), vmem_spec()),
        cost_estimate=pl.CostEstimate(flops=1000, bytes_accessed=4 << 20, transcendentals=0),
        name="pack",
    )(sel, key_heads, values)
    remote = lax.all_to_all(outgoing, "kv", split_axis=0, concat_axis=0, tiled=True)
    whole = lax.all_to_all(
        jnp.broadcast_to(inputs[None], (4, *inputs.shape)), "tp", 0, 0, tiled=True
    )

    def by_block(array):
        array = array.reshape(BLOCKS, BLOCK, GROUPS, PER_GROUP, HD)
        return array.transpose(2, 0, 3, 1, 4).reshape(GROUPS * BLOCKS, COLS, HD)

    none = ((0, 0), (0, 0))
    query = jnp.pad(by_block(queries), (*none, (0, HD)))
    grad = jnp.pad(by_block(out_grad), (*none, (HD, 0)))
    sums = log_sums.reshape(GROUPS, PER_GROUP, BLOCKS, BLOCK).transpose(0, 2, 1, 3)
    sums = sums.reshape(GROUPS * BLOCKS, 1, COLS) * LOG2E

    sent, kept, query_grad = pl.pallas_call(
        attention_kernel,
        out_shape=(
            jax.ShapeDtypeStruct((DEVS, GROUPS, BLOCK, 2 * HD), bf16),
            jax.ShapeDtypeStruct((GROUPS, BLOCKS, BLOCK, 2 * HD), jnp.float32),
            jax.ShapeDtypeStruct((GROUPS * BLOCKS, HD, COLS), jnp.float32),
        ),
        in_specs=[smem_spec(), smem_spec(), *[vmem_spec()] * 5],
        out_specs=(vmem_spec(), vmem_spec(), vmem_spec()),
        scratch_shapes=[
            VMEM((DEVS + BLOCKS, GROUPS, BLOCK, 2 * HD), jnp.float32),
            VMEM((LIST * BLOCK, 2 * HD), bf16),
            VMEM((LIST * BLOCK, COLS), jnp.float32),
            VMEM((LIST * BLOCK, COLS), jnp.float32),
        ],
        cost_estimate=pl.CostEstimate(
            flops=4 << 30, bytes_accessed=8 << 20, transcendentals=3 << 20
        ),
        name="attention",
    )(slot, near, remote, own, query, grad, sums)
    returned = lax.all_to_all(sent, "kv", split_axis=0, concat_axis=0, tiled=True)
    query_grad = query_grad.reshape(GROUPS, BLOCKS, HD, PER_GROUP, BLOCK)
    query_grad = query_grad.transpose(1, 4, 0, 3, 2).reshape(rows, GROUPS * PER_GROUP * HD)

    key_grad, value_grad, key_half = pl.pallas_call(
        collect_kernel,
        out_shape=(
            jax.ShapeDtypeStruct((rows, 2 * HD), jnp.float32),
            jax.ShapeDtypeStruct((rows, 2 * HD), jnp.float32),
            jax.ShapeDtypeStruct((rows, 2 * HD), bf16),
        ),
        in_specs=[smem_spec(), vmem_spec(), vmem_spec()],
        out_specs=(vmem_spec(), vmem_spec(), vmem_spec()),
        scratch_shapes=[VMEM((GROUPS, BLOCKS, BLOCK, 2 * HD), jnp.float32)],
        cost_estimate=pl.CostEstimate(flops=2 << 20, bytes_accessed=4 << 20, transcendentals=0),
        name="collect",
    )(sel, returned, kept)
    terms = jnp.einsum("xtf,tc->xfc", whole, key_half, preferred_element_type=jnp.float32)
    terms = terms.astype(bf16).reshape(DEVS, BLOCK, 2 * HD)
    arrived = lax.all_to_all(terms, "kv", split_axis=0, concat_axis=0, tiled=True)
    weight_grad = arrived.astype(jnp.float32).sum(axis=0)
    return (query_grad, key_grad, value_grad, weight_grad)


def solution(mesh):
    placed = (
        P("kv", "tp"),
        P("kv", "tp"),
        P("kv", "tp"),
        P("tp", "kv"),
        P("kv", "tp"),
        P("kv", "tp"),
        P("tp", None, None),
    )
    return jax.shard_map(
        local,
        mesh=mesh,
        in_specs=placed,
        out_specs=(P("kv", "tp"), P("kv", "tp"), P("kv", "tp"), P("kv", "tp")),
        check_vma=False,
    )
```

```python
import jax
import jax.numpy as jnp
from jax import lax
from jax.experimental import pallas as pl
from jax.experimental.pallas import tpu as pltpu
from jax.sharding import PartitionSpec as P

HD = 64
BLOCK = 64
GROUPS = 2
PER_GROUP = 4
BLOCKS = 6
LIST = 16
DEVS = 64
TP = 4
COLS = PER_GROUP * BLOCK
CHUNK = 256
LOG2E = 1.4426950408889634
VMEM = pltpu.VMEM
SMEM = pltpu.SMEM


def vmem_spec():
    return pl.BlockSpec(memory_space=VMEM)


def smem_spec():
    return pl.BlockSpec(memory_space=SMEM)


def pack_kernel(sel_ref, keys_ref, values_ref, out_ref, own_ref):
    shape = (BLOCKS * BLOCK, 2 * HD)
    low = lax.broadcasted_iota(jnp.int32, shape, 1) < HD
    keys = keys_ref[...].astype(jnp.float32)
    values = values_ref[...].astype(jnp.float32)
    first = jnp.where(low, keys, pltpu.roll(values, HD, 1)).astype(jnp.bfloat16)
    second = jnp.where(low, pltpu.roll(keys, HD, 1), values).astype(jnp.bfloat16)
    own_ref[0] = first.reshape(BLOCKS, BLOCK, 2 * HD)
    own_ref[1] = second.reshape(BLOCKS, BLOCK, 2 * HD)

    @pl.loop(0, DEVS)
    def _(dest):
        for group in range(GROUPS):
            out_ref[dest, group] = own_ref[group, sel_ref[group, dest]]


def dot(a, b, dims):
    return lax.dot_general(a, b, (dims, ((), ())), preferred_element_type=jnp.float32)


def attention_kernel(
    slot_ref,
    near_ref,
    remote_ref,
    own_ref,
    query_ref,
    grad_ref,
    sums_ref,
    sent_ref,
    kept_ref,
    query_grad_ref,
    totals,
    *scratch,
):
    totals[...] = jnp.zeros_like(totals)
    rows = lax.broadcasted_iota(jnp.int32, (BLOCK, COLS), 0)
    cols = lax.broadcasted_iota(jnp.int32, (BLOCK, COLS), 1)
    behind = rows - (cols & (BLOCK - 1))
    per_chunk = CHUNK // BLOCK
    even, odd = scratch[:4], scratch[4:]

    def first_pass(step, held, chunk, delta):
        table, probs, prob_grads, _ = held
        group = step // BLOCKS
        sums = sums_ref[step]
        entries = range(chunk * per_chunk, (chunk + 1) * per_chunk)
        for entry in entries:
            slot = slot_ref[step, entry]
            far = remote_ref[jnp.minimum(slot, DEVS - 1), group]
            close = own_ref[group, jnp.maximum(slot - DEVS, 0)]
            table[pl.ds(entry * BLOCK, BLOCK), :] = jnp.where(slot < DEVS, far, close)
        pair = table[pl.ds(chunk * CHUNK, CHUNK), :]
        scores = dot(pair, query_ref[step], ((1,), (1,)))
        grads = dot(pair, grad_ref[step], ((1,), (1,)))
        for inner, entry in enumerate(entries):
            part = slice(inner * BLOCK, (inner + 1) * BLOCK)
            prob = jnp.exp2(scores[part] * (LOG2E * HD**-0.5) - sums)
            prob = jnp.where(behind <= near_ref[step, entry], prob, 0.0)
            delta = delta + jnp.sum((prob * grads[part]).reshape(8, 8, COLS), axis=0)
            probs[pl.ds(entry * BLOCK, BLOCK), :] = prob
            prob_grads[pl.ds(entry * BLOCK, BLOCK), :] = grads[part]
        return delta

    def second_pass(step, held, chunk, query_grad):
        table, probs, prob_grads, delta = held
        group = step // BLOCKS
        part = pl.ds(chunk * CHUNK, CHUNK)
        prob = probs[part, :]
        score_grad = (prob * (prob_grads[part, :] - delta[...])).astype(jnp.bfloat16)
        contrib = dot(score_grad, query_ref[step], ((1,), (0,)))
        contrib = contrib + dot(prob.astype(jnp.bfloat16), grad_ref[step], ((1,), (0,)))
        for inner in range(per_chunk):
            slot = slot_ref[step, chunk * per_chunk + inner]
            totals[slot, group] += contrib[inner * BLOCK : (inner + 1) * BLOCK]
        return query_grad + dot(table[part, :], score_grad, ((0,), (0,)))

    def passes(first=None, second=None):
        delta = jnp.zeros((8, COLS), jnp.float32)
        query_grad = jnp.zeros((2 * HD, COLS), jnp.float32)
        for chunk in range(LIST * BLOCK // CHUNK):
            if first is not None:
                delta = first_pass(*first, chunk, delta)
            if second is not None:
                query_grad = second_pass(*second, chunk, query_grad)
        if first is not None:
            first[1][3][...] = jnp.sum(delta, axis=0, keepdims=True)
        if second is not None:
            query_grad_ref[second[0]] = query_grad[:HD] * HD**-0.5

    last = GROUPS * BLOCKS - 1
    passes(first=(0, even))

    @pl.loop(0, last // 2)
    def _(i):
        passes(first=(2 * i + 1, odd), second=(2 * i, even))
        passes(first=(2 * i + 2, even), second=(2 * i + 1, odd))

    passes(first=(last, odd), second=(last - 1, even))
    passes(second=(last, odd))

    lane = lax.broadcasted_iota(jnp.int32, (BLOCK, 2 * HD), 1)
    factor = jnp.where(lane < HD, HD**-0.5, 1.0)

    @pl.loop(0, DEVS, unroll=4)
    def _(dest):
        for group in range(GROUPS):
            sent_ref[dest, group] = (totals[dest, group] * factor).astype(jnp.bfloat16)

    for block in range(BLOCKS):
        for group in range(GROUPS):
            kept_ref[group, block] = totals[DEVS + block, group] * factor


def collect_kernel(sel_ref, returned_ref, kept_ref, key_ref, value_ref, half_ref, total):
    total[...] = kept_ref[...]

    @pl.loop(0, DEVS)
    def _(source):
        for group in range(GROUPS):
            total[group, sel_ref[group, source]] += returned_ref[source, group].astype(jnp.float32)

    low = lax.broadcasted_iota(jnp.int32, (BLOCKS * BLOCK, 2 * HD), 1) < HD
    first = total[0].reshape(BLOCKS * BLOCK, 2 * HD)
    second = total[1].reshape(BLOCKS * BLOCK, 2 * HD)
    key_grad = jnp.where(low, first, pltpu.roll(second, HD, 1))
    key_ref[...] = key_grad
    half_ref[...] = key_grad.astype(jnp.bfloat16)
    value_ref[...] = jnp.where(low, pltpu.roll(first, HD, 1), second)


def weight_kernel(tp_ref, key_ref, *refs):
    *pieces, out_ref = refs
    for shift, piece in enumerate(pieces):
        terms = dot(piece[...], key_ref[...], ((1,), (0,)))
        out_ref[lax.rem(tp_ref[0] + TP - shift, TP)] = terms.astype(jnp.bfloat16)


def local(queries, key_heads, values, log_sums, out_grad, inputs, chosen):
    me = lax.axis_index("kv")
    rows = BLOCKS * BLOCK
    first = me * BLOCKS
    within = chosen.reshape(GROUPS, DEVS, BLOCKS * LIST) - first
    listed = (within >= 0) & (within < BLOCKS)
    sel = jnp.max(jnp.where(listed, within, 0), axis=2)
    mine = lax.dynamic_slice_in_dim(chosen, first, BLOCKS, 1)
    near = mine - first
    slot = jnp.where(near >= 0, DEVS + near, jnp.maximum(mine, 0) // BLOCKS)
    positions = jnp.arange(BLOCKS, dtype=jnp.int32)[None, :, None]
    near = jnp.where(mine < 0, -BLOCK, jnp.where(near == positions, 0, BLOCK))
    slot = slot.reshape(GROUPS * BLOCKS, LIST)
    near = near.reshape(GROUPS * BLOCKS, LIST)

    bf16 = jnp.bfloat16
    outgoing, own = pl.pallas_call(
        pack_kernel,
        out_shape=(
            jax.ShapeDtypeStruct((DEVS, GROUPS, BLOCK, 2 * HD), bf16),
            jax.ShapeDtypeStruct((GROUPS, BLOCKS, BLOCK, 2 * HD), bf16),
        ),
        in_specs=[smem_spec(), vmem_spec(), vmem_spec()],
        out_specs=(vmem_spec(), vmem_spec()),
        cost_estimate=pl.CostEstimate(flops=1000, bytes_accessed=4 << 20, transcendentals=0),
        name="pack",
    )(sel, key_heads, values)
    remote = lax.all_to_all(outgoing, "kv", split_axis=0, concat_axis=0, tiled=True)
    core = me % 2
    halves = inputs.reshape(rows, 8, 2, HD)
    mine, theirs = (
        jnp.where(core == parity, halves[:, :, 0], halves[:, :, 1]).reshape(rows, 8 * HD)
        for parity in range(2)
    )
    partner = [(i, i ^ 1) for i in range(DEVS)]
    features = jnp.concatenate([mine, lax.ppermute(theirs, "kv", partner)], axis=0).T
    pieces = [features]
    for shift in range(1, TP):
        ring = [(i, (i + shift) % TP) for i in range(TP)]
        pieces.append(lax.ppermute(features, "tp", ring))

    def by_block(array):
        array = array.reshape(BLOCKS, BLOCK, GROUPS, PER_GROUP, HD)
        return array.transpose(2, 0, 3, 1, 4).reshape(GROUPS * BLOCKS, COLS, HD)

    none = ((0, 0), (0, 0))
    query = jnp.pad(by_block(queries), (*none, (0, HD)))
    grad = jnp.pad(by_block(out_grad), (*none, (HD, 0)))
    sums = log_sums.reshape(GROUPS, PER_GROUP, BLOCKS, BLOCK).transpose(0, 2, 1, 3)
    sums = sums.reshape(GROUPS * BLOCKS, 1, COLS) * LOG2E

    held = [
        VMEM((LIST * BLOCK, 2 * HD), bf16),
        VMEM((LIST * BLOCK, COLS), jnp.float32),
        VMEM((LIST * BLOCK, COLS), jnp.float32),
        VMEM((1, COLS), jnp.float32),
    ]
    sent, kept, query_grad = pl.pallas_call(
        attention_kernel,
        out_shape=(
            jax.ShapeDtypeStruct((DEVS, GROUPS, BLOCK, 2 * HD), bf16),
            jax.ShapeDtypeStruct((GROUPS, BLOCKS, BLOCK, 2 * HD), jnp.float32),
            jax.ShapeDtypeStruct((GROUPS * BLOCKS, HD, COLS), jnp.float32),
        ),
        in_specs=[smem_spec(), smem_spec(), *[vmem_spec()] * 5],
        out_specs=(vmem_spec(), vmem_spec(), vmem_spec()),
        scratch_shapes=[
            VMEM((DEVS + BLOCKS, GROUPS, BLOCK, 2 * HD), jnp.float32),
            *held,
            *held,
        ],
        cost_estimate=pl.CostEstimate(
            flops=4 << 30, bytes_accessed=8 << 20, transcendentals=3 << 20
        ),
        name="attention",
    )(slot, near, remote, own, query, grad, sums)
    returned = lax.all_to_all(sent, "kv", split_axis=0, concat_axis=0, tiled=True)
    query_grad = query_grad.reshape(GROUPS, BLOCKS, HD, PER_GROUP, BLOCK)
    query_grad = query_grad.transpose(1, 4, 0, 3, 2).reshape(rows, GROUPS * PER_GROUP * HD)

    key_grad, value_grad, key_half = pl.pallas_call(
        collect_kernel,
        out_shape=(
            jax.ShapeDtypeStruct((rows, 2 * HD), jnp.float32),
            jax.ShapeDtypeStruct((rows, 2 * HD), jnp.float32),
            jax.ShapeDtypeStruct((rows, 2 * HD), bf16),
        ),
        in_specs=[smem_spec(), vmem_spec(), vmem_spec()],
        out_specs=(vmem_spec(), vmem_spec(), vmem_spec()),
        scratch_shapes=[VMEM((GROUPS, BLOCKS, BLOCK, 2 * HD), jnp.float32)],
        cost_estimate=pl.CostEstimate(flops=2 << 20, bytes_accessed=4 << 20, transcendentals=0),
        name="collect",
    )(sel, returned, kept)
    key_pair = jnp.concatenate([key_half, lax.ppermute(key_half, "kv", partner)], axis=0)
    terms = pl.pallas_call(
        weight_kernel,
        out_shape=jax.ShapeDtypeStruct((TP, 8 * HD, 2 * HD), bf16),
        in_specs=[smem_spec(), *[vmem_spec()] * 5],
        out_specs=vmem_spec(),
        cost_estimate=pl.CostEstimate(flops=1 << 29, bytes_accessed=4 << 20, transcendentals=0),
        name="weights",
    )(lax.axis_index("tp").reshape(1), key_pair, *pieces)
    same_core = [list(range(parity, DEVS, 2)) for parity in range(2)]
    terms = terms.reshape(DEVS // 2, HD, 2 * HD)
    arrived = lax.all_to_all(terms, "kv", 0, 0, tiled=True, axis_index_groups=same_core)
    weight_grad = arrived.astype(jnp.float32).sum(axis=0)
    return (query_grad, key_grad, value_grad, weight_grad)


def solution(mesh):
    placed = (
        P("kv", "tp"),
        P("kv", "tp"),
        P("kv", "tp"),
        P("tp", "kv"),
        P("kv", "tp"),
        P("kv", "tp"),
        P("tp", None, None),
    )
    return jax.shard_map(
        local,
        mesh=mesh,
        in_specs=placed,
        out_specs=(P("kv", "tp"), P("kv", "tp"), P("kv", "tp"), P("kv", "tp")),
        check_vma=False,
    )
```

```python
import jax
import jax.numpy as jnp
from jax import lax
from jax.experimental import pallas as pl
from jax.experimental.pallas import tpu as pltpu
from jax.sharding import PartitionSpec as P

HD = 64
BLOCK = 64
GROUPS = 2
PER_GROUP = 4
BLOCKS = 6
LIST = 16
DEVS = 64
TP = 4
COLS = PER_GROUP * BLOCK
CHUNK = 1024
PACKED = 16
STREAMS = 8
LOG2E = 1.4426950408889634
VMEM = pltpu.VMEM
SMEM = pltpu.SMEM


def vmem_spec():
    return pl.BlockSpec(memory_space=VMEM)


def any_spec():
    return pl.BlockSpec(memory_space=pl.ANY)


def smem_spec():
    return pl.BlockSpec(memory_space=SMEM)


def pack_kernel(sel_ref, keys_ref, values_ref, out_ref, own_ref):
    @pl.when(pl.program_id(0) == 0)
    def _():
        low = lax.broadcasted_iota(jnp.int32, (BLOCKS * BLOCK, 2 * HD), 1) < HD
        keys = keys_ref[...].astype(jnp.float32)
        values = values_ref[...].astype(jnp.float32)
        first = jnp.where(low, keys, pltpu.roll(values, HD, 1)).astype(jnp.bfloat16)
        second = jnp.where(low, pltpu.roll(keys, HD, 1), values).astype(jnp.bfloat16)
        own_ref[0] = first.reshape(BLOCKS, BLOCK, 2 * HD)
        own_ref[1] = second.reshape(BLOCKS, BLOCK, 2 * HD)

    for inner in range(PACKED):
        dest = pl.program_id(0) * PACKED + inner
        for group in range(GROUPS):
            out_ref[inner, group] = own_ref[group, sel_ref[group, dest]]


def dot(a, b, dims):
    return lax.dot_general(a, b, (dims, ((), ())), preferred_element_type=jnp.float32)


def attention_kernel(
    slot_ref,
    near_ref,
    remote_ref,
    own_ref,
    query_ref,
    grad_ref,
    sums_ref,
    sent_ref,
    kept_ref,
    query_grad_ref,
    totals,
    *scratch,
):
    totals[...] = jnp.zeros_like(totals)
    rows = lax.broadcasted_iota(jnp.int32, (BLOCK, COLS), 0)
    cols = lax.broadcasted_iota(jnp.int32, (BLOCK, COLS), 1)
    behind = rows - (cols & (BLOCK - 1))
    per_chunk = CHUNK // BLOCK
    even, odd = scratch[:4], scratch[4:]

    def first_pass(step, held, chunk, delta):
        table, probs, prob_grads, _ = held
        group = step // BLOCKS
        sums = sums_ref[step]
        entries = range(chunk * per_chunk, (chunk + 1) * per_chunk)
        for entry in entries:
            slot = slot_ref[step, entry]
            far = remote_ref[jnp.minimum(slot, DEVS - 1), group]
            close = own_ref[group, jnp.maximum(slot - DEVS, 0)]
            table[pl.ds(entry * BLOCK, BLOCK), :] = jnp.where(slot < DEVS, far, close)
        pair = table[pl.ds(chunk * CHUNK, CHUNK), :]
        scores = dot(pair, query_ref[step], ((1,), (1,)))
        grads = dot(pair, grad_ref[step], ((1,), (1,)))
        for inner, entry in enumerate(entries):
            part = slice(inner * BLOCK, (inner + 1) * BLOCK)
            prob = jnp.exp2(scores[part] * (LOG2E * HD**-0.5) - sums)
            prob = jnp.where(behind <= near_ref[step, entry], prob, 0.0)
            delta = delta + jnp.sum((prob * grads[part]).reshape(8, 8, COLS), axis=0)
            probs[pl.ds(entry * BLOCK, BLOCK), :] = prob
            prob_grads[pl.ds(entry * BLOCK, BLOCK), :] = grads[part]
        return delta

    def second_pass(step, held, chunk, query_grad):
        table, probs, prob_grads, delta = held
        group = step // BLOCKS
        part = pl.ds(chunk * CHUNK, CHUNK)
        prob = probs[part, :]
        score_grad = (prob * (prob_grads[part, :] - delta[...])).astype(jnp.bfloat16)
        contrib = dot(score_grad, query_ref[step], ((1,), (0,)))
        contrib = contrib + dot(prob.astype(jnp.bfloat16), grad_ref[step], ((1,), (0,)))
        for inner in range(per_chunk):
            slot = slot_ref[step, chunk * per_chunk + inner]
            totals[slot, group] += contrib[inner * BLOCK : (inner + 1) * BLOCK]
        return query_grad + dot(table[part, :HD], score_grad, ((0,), (0,)))

    def passes(first=None, second=None):
        delta = jnp.zeros((8, COLS), jnp.float32)
        query_grad = jnp.zeros((HD, COLS), jnp.float32)
        for chunk in range(LIST * BLOCK // CHUNK):
            if first is not None:
                delta = first_pass(*first, chunk, delta)
            if second is not None:
                query_grad = second_pass(*second, chunk, query_grad)
        if first is not None:
            first[1][3][...] = jnp.sum(delta, axis=0, keepdims=True)
        if second is not None:
            query_grad_ref[second[0]] = query_grad * HD**-0.5

    last = GROUPS * BLOCKS - 1
    passes(first=(0, even))

    @pl.loop(0, last // 2)
    def _(i):
        passes(first=(2 * i + 1, odd), second=(2 * i, even))
        passes(first=(2 * i + 2, even), second=(2 * i + 1, odd))

    passes(first=(last, odd), second=(last - 1, even))
    passes(second=(last, odd))

    lane = lax.broadcasted_iota(jnp.int32, (BLOCK, 2 * HD), 1)
    factor = jnp.where(lane < HD, HD**-0.5, 1.0)

    @pl.loop(0, DEVS, unroll=4)
    def _(dest):
        for group in range(GROUPS):
            sent_ref[dest, group] = (totals[dest, group] * factor).astype(jnp.bfloat16)

    for block in range(BLOCKS):
        for group in range(GROUPS):
            kept_ref[group, block] = totals[DEVS + block, group] * factor


def collect_kernel(
    sel_ref, returned_any, kept_ref, key_ref, value_ref, half_ref, total, returned, sems
):
    peers = DEVS // STREAMS
    copies = [
        pltpu.make_async_copy(
            returned_any.at[pl.ds(stream * peers, peers)],
            returned.at[pl.ds(stream * peers, peers)],
            sems.at[stream],
        )
        for stream in range(STREAMS)
    ]
    for copy in copies:
        copy.start()
    total[...] = kept_ref[...]
    for stream, copy in enumerate(copies):
        copy.wait()
        for source in range(stream * peers, (stream + 1) * peers):
            for group in range(GROUPS):
                block = sel_ref[group, source]
                total[group, block] += returned[source, group].astype(jnp.float32)

    low = lax.broadcasted_iota(jnp.int32, (BLOCKS * BLOCK, 2 * HD), 1) < HD
    first = total[0].reshape(BLOCKS * BLOCK, 2 * HD)
    second = total[1].reshape(BLOCKS * BLOCK, 2 * HD)
    key_grad = jnp.where(low, first, pltpu.roll(second, HD, 1))
    key_ref[...] = key_grad
    half_ref[...] = key_grad.astype(jnp.bfloat16)
    value_ref[...] = jnp.where(low, pltpu.roll(first, HD, 1), second)


def weight_kernel(tp_ref, near_ref, far_ref, *refs):
    pieces, (out_ref, held, sems) = refs[:TP], refs[TP:]
    rows = BLOCKS * BLOCK
    copies = [
        pltpu.make_async_copy(piece, held.at[shift], sems.at[shift])
        for shift, piece in enumerate(pieces)
    ]
    for copy in copies:
        copy.start()
    for shift, copy in enumerate(copies):
        copy.wait()
        terms = dot(held[shift, :, :rows], near_ref[...], ((1,), (0,)))
        terms = terms + dot(held[shift, :, rows:], far_ref[...], ((1,), (0,)))
        out_ref[lax.rem(tp_ref[0] + TP - shift, TP)] = terms.astype(jnp.bfloat16)


def local(queries, key_heads, values, log_sums, out_grad, inputs, chosen):
    me = lax.axis_index("kv")
    rows = BLOCKS * BLOCK
    first = me * BLOCKS
    within = chosen.reshape(GROUPS, DEVS, BLOCKS * LIST) - first
    listed = (within >= 0) & (within < BLOCKS)
    sel = jnp.max(jnp.where(listed, within, 0), axis=2)
    mine = lax.dynamic_slice_in_dim(chosen, first, BLOCKS, 1)
    near = mine - first
    slot = jnp.where(near >= 0, DEVS + near, jnp.maximum(mine, 0) // BLOCKS)
    positions = jnp.arange(BLOCKS, dtype=jnp.int32)[None, :, None]
    near = jnp.where(mine < 0, -BLOCK, jnp.where(near == positions, 0, BLOCK))
    slot = slot.reshape(GROUPS * BLOCKS, LIST)
    near = near.reshape(GROUPS * BLOCKS, LIST)

    bf16 = jnp.bfloat16
    outgoing, own = pl.pallas_call(
        pack_kernel,
        out_shape=(
            jax.ShapeDtypeStruct((DEVS, GROUPS, BLOCK, 2 * HD), bf16),
            jax.ShapeDtypeStruct((GROUPS, BLOCKS, BLOCK, 2 * HD), bf16),
        ),
        grid=(DEVS // PACKED,),
        in_specs=[
            smem_spec(),
            pl.BlockSpec((rows, 2 * HD), lambda i: (0, 0)),
            pl.BlockSpec((rows, 2 * HD), lambda i: (0, 0)),
        ],
        out_specs=(
            pl.BlockSpec((PACKED, GROUPS, BLOCK, 2 * HD), lambda i: (i, 0, 0, 0)),
            pl.BlockSpec((GROUPS, BLOCKS, BLOCK, 2 * HD), lambda i: (0, 0, 0, 0)),
        ),
        cost_estimate=pl.CostEstimate(flops=1000, bytes_accessed=4 << 20, transcendentals=0),
        name="pack",
    )(sel, key_heads, values)
    remote = lax.all_to_all(outgoing, "kv", split_axis=0, concat_axis=0, tiled=True)
    core = me % 2
    halves = inputs.reshape(rows, 8, 2, HD)
    mine, theirs = (
        jnp.where(core == parity, halves[:, :, 0], halves[:, :, 1]).reshape(rows, 8 * HD)
        for parity in range(2)
    )
    partner = [(i, i ^ 1) for i in range(DEVS)]
    features = jnp.concatenate([mine, lax.ppermute(theirs, "kv", partner)], axis=0).T
    pieces = [features]
    for shift in range(1, TP):
        ring = [(i, (i + shift) % TP) for i in range(TP)]
        pieces.append(lax.ppermute(features, "tp", ring))

    def by_block(array):
        array = array.reshape(BLOCKS, BLOCK, GROUPS, PER_GROUP, HD)
        return array.transpose(2, 0, 3, 1, 4).reshape(GROUPS * BLOCKS, COLS, HD)

    none = ((0, 0), (0, 0))
    query = jnp.pad(by_block(queries), (*none, (0, HD)))
    grad = jnp.pad(by_block(out_grad), (*none, (HD, 0)))
    sums = log_sums.reshape(GROUPS, PER_GROUP, BLOCKS, BLOCK).transpose(0, 2, 1, 3)
    sums = sums.reshape(GROUPS * BLOCKS, 1, COLS) * LOG2E

    held = [
        VMEM((LIST * BLOCK, 2 * HD), bf16),
        VMEM((LIST * BLOCK, COLS), jnp.float32),
        VMEM((LIST * BLOCK, COLS), jnp.float32),
        VMEM((1, COLS), jnp.float32),
    ]
    sent, kept, query_grad = pl.pallas_call(
        attention_kernel,
        out_shape=(
            jax.ShapeDtypeStruct((DEVS, GROUPS, BLOCK, 2 * HD), bf16),
            jax.ShapeDtypeStruct((GROUPS, BLOCKS, BLOCK, 2 * HD), jnp.float32),
            jax.ShapeDtypeStruct((GROUPS * BLOCKS, HD, COLS), jnp.float32),
        ),
        in_specs=[smem_spec(), smem_spec(), *[vmem_spec()] * 5],
        out_specs=(vmem_spec(), vmem_spec(), vmem_spec()),
        scratch_shapes=[
            VMEM((DEVS + BLOCKS, GROUPS, BLOCK, 2 * HD), jnp.float32),
            *held,
            *held,
        ],
        cost_estimate=pl.CostEstimate(
            flops=4 << 30, bytes_accessed=8 << 20, transcendentals=3 << 20
        ),
        name="attention",
    )(slot, near, remote, own, query, grad, sums)
    returned = lax.all_to_all(sent, "kv", split_axis=0, concat_axis=0, tiled=True)
    query_grad = query_grad.reshape(GROUPS, BLOCKS, HD, PER_GROUP, BLOCK)
    query_grad = query_grad.transpose(1, 4, 0, 3, 2).reshape(rows, GROUPS * PER_GROUP * HD)

    key_grad, value_grad, key_half = pl.pallas_call(
        collect_kernel,
        out_shape=(
            jax.ShapeDtypeStruct((rows, 2 * HD), jnp.float32),
            jax.ShapeDtypeStruct((rows, 2 * HD), jnp.float32),
            jax.ShapeDtypeStruct((rows, 2 * HD), bf16),
        ),
        in_specs=[smem_spec(), any_spec(), vmem_spec()],
        out_specs=(vmem_spec(), vmem_spec(), vmem_spec()),
        scratch_shapes=[
            VMEM((GROUPS, BLOCKS, BLOCK, 2 * HD), jnp.float32),
            VMEM((DEVS, GROUPS, BLOCK, 2 * HD), bf16),
            pltpu.SemaphoreType.DMA((STREAMS,)),
        ],
        compiler_params=pltpu.CompilerParams(vmem_limit_bytes=24 << 20),
        cost_estimate=pl.CostEstimate(flops=2 << 20, bytes_accessed=4 << 20, transcendentals=0),
        name="collect",
    )(sel, returned, kept)
    key_far = lax.ppermute(key_half, "kv", partner)
    terms = pl.pallas_call(
        weight_kernel,
        out_shape=jax.ShapeDtypeStruct((TP, 8 * HD, 2 * HD), bf16),
        in_specs=[smem_spec(), vmem_spec(), vmem_spec(), *[any_spec()] * TP],
        out_specs=vmem_spec(),
        scratch_shapes=[
            VMEM((TP, 8 * HD, 2 * rows), bf16),
            pltpu.SemaphoreType.DMA((TP,)),
        ],
        compiler_params=pltpu.CompilerParams(vmem_limit_bytes=24 << 20),
        cost_estimate=pl.CostEstimate(flops=1 << 29, bytes_accessed=4 << 20, transcendentals=0),
        name="weights",
    )(lax.axis_index("tp").reshape(1), key_half, key_far, *pieces)
    same_core = [list(range(parity, DEVS, 2)) for parity in range(2)]
    terms = terms.reshape(DEVS // 2, HD, 2 * HD)
    arrived = lax.all_to_all(terms, "kv", 0, 0, tiled=True, axis_index_groups=same_core)
    weight_grad = arrived.astype(jnp.float32).sum(axis=0)
    return (query_grad, key_grad, value_grad, weight_grad)


def solution(mesh):
    placed = (
        P("kv", "tp"),
        P("kv", "tp"),
        P("kv", "tp"),
        P("tp", "kv"),
        P("kv", "tp"),
        P("kv", "tp"),
        P("tp", None, None),
    )
    return jax.shard_map(
        local,
        mesh=mesh,
        in_specs=placed,
        out_specs=(P("kv", "tp"), P("kv", "tp"), P("kv", "tp"), P("kv", "tp")),
        check_vma=False,
    )
```
